32 devices in a mesh: fs: 4 (over z), rep: 4 (over y, x), tp: 2 (over core).
Axes of the slice: x: 2, y: 2, z: 4, core: 2. Of those that a mesh axis runs over, the one named last changes fastest.
Arguments:
- query_input: bfloat16 [16384, 4096], P(('fs', 'rep')), may hold values from -6 to 6
- query_cotangent: bfloat16 [16384, 1024], P(('fs', 'rep'), 'tp'), may hold values from -0.046875 to 0.046875
- branch_output: bfloat16 [16384, 2048], P(('fs', 'rep')), may hold values from -6 to 6
- layer_cotangent: bfloat16 [16384, 4096], P(('fs', 'rep'), 'tp'), may hold values from -0.046875 to 0.046875
- query_weight: float32 [4096, 1024], P(('rep', 'fs'), 'tp'), may hold values from -0.09375 to 0.09375
- output_weight: float32 [2048, 4096], P(('rep', 'fs'), 'tp'), may hold values from -0.125 to 0.125
- query_basis: bfloat16 [4096, 512], P(('rep', 'fs')), may hold values from -0.09375 to 0.09375
- output_basis: bfloat16 [2048, 512], P(('rep', 'fs')), may hold values from -0.125 to 0.125
- query_first: float32 [512, 1024], P(('rep', 'fs'), 'tp'), may hold values from -20 to 20
- query_second: float32 [512, 1024], P(('rep', 'fs'), 'tp'), may hold values from 0.25 to 2
- output_first: float32 [512, 4096], P(('rep', 'fs'), 'tp'), may hold values from -20 to 20
- output_second: float32 [512, 4096], P(('rep', 'fs'), 'tp'), may hold values from 0.25 to 2
Outputs:
- query_update: float32 [4096, 1024], P(('rep', 'fs'), 'tp')
- output_update: float32 [2048, 4096], P(('rep', 'fs'), 'tp')
- query_first_next: float32 [512, 1024], P(('rep', 'fs'), 'tp')
- query_second_next: float32 [512, 1024], P(('rep', 'fs'), 'tp')
- output_first_next: float32 [512, 4096], P(('rep', 'fs'), 'tp')
- output_second_next: float32 [512, 4096], P(('rep', 'fs'), 'tp')
- query_copy: bfloat16 [4096, 1024], P('rep', 'tp')
- output_copy: bfloat16 [2048, 4096], P('rep', 'tp')
The draws below stay inside these ranges and needn't reach their ends.
All inputs are finite; a program needn't handle non-finite values.
Results may differ from the reference program's by a relative error of at most 0.0055.
Values may be sent and summed in bfloat16 or wider, within the bound.
A program may use at most 128 MiB of HBM per device.

```python
import math
import jax
import jax.numpy as jnp
from jax import lax

D = 4096
QKW = 1024
VW = 2048
R = 512
TOKENS = 16384


def first_moment(key, rows, cols):
    row_scale = 0.3 * 10.0 ** (jnp.arange(rows, dtype=jnp.float32) / (rows - 1))
    col_scale = jnp.exp(jax.random.uniform(jax.random.fold_in(key, 7), (cols,), jnp.float32, -0.7, 0.7))
    base = jnp.clip(jax.random.normal(jax.random.fold_in(key, 11), (rows, cols), jnp.float32), -3.0, 3.0)
    return base * row_scale[:, None] * col_scale[None, :]


def draw_query_first(key, part):
    return first_moment(key, R, QKW)


def draw_output_first(key, part):
    return first_moment(key, R, D)


def level_of(stream_key, extent, split, low, high):
    def one(dim, blocks):
        heights = jax.random.uniform(jax.random.fold_in(jax.random.fold_in(stream_key, 6), dim), (blocks,), jnp.float32, low / len(split), high / len(split))
        return jnp.repeat(jnp.exp(heights), extent[dim] // blocks).reshape((-1,) + (1,) * (len(extent) - dim - 1))

    loudness = one(*split[0])
    for cut in split[1:]:
        loudness = loudness * one(*cut)
    return loudness


def scatter_about(stream_key, dims, spread, reach, shards=(), kind=jnp.bfloat16):
    result = spread * jax.random.normal(stream_key, dims, jnp.float32)
    if shards:
        result = result * level_of(stream_key, dims, shards, -0.22, 0.18)
    return jnp.clip(result, -reach, reach).astype(kind)


def setup_inputs(seed: int = 0) -> dict:
    keys = jax.random.split(jax.random.key(seed), 13)
    query_input = scatter_about(keys[0], (TOKENS, D), 1.0, 6.0, ((0, 16),))
    query_cotangent = scatter_about(keys[1], (TOKENS, QKW), (TOKENS ** -0.5), 0.046875, ((0, 16), (1, 2)))
    branch_output = scatter_about(keys[2], (TOKENS, VW), 1.0, 6.0, ((0, 16),))
    layer_cotangent = scatter_about(keys[3], (TOKENS, D), (TOKENS ** -0.5), 0.046875, ((0, 16), (1, 2)))
    query_weight = scatter_about(keys[4], (D, QKW), D ** -0.5, 0.09375, ((0, 16), (1, 2)), jnp.float32)
    output_weight = scatter_about(keys[5], (VW, D), VW ** -0.5, 0.125, ((0, 16), (1, 2)), jnp.float32)
    query_basis = scatter_about(keys[6], (D, R), D ** -0.5, 0.09375, ((0, 16),))
    output_basis = scatter_about(keys[7], (VW, R), VW ** -0.5, 0.125, ((0, 16),))
    query_first = draw_query_first(jax.random.fold_in(keys[12], 71), 0)
    query_second = jnp.clip(jnp.exp(math.log(2.0) - 2.0794415 * jax.random.uniform(keys[9], (R, QKW), jnp.float32) ** level_of(keys[9], (R, QKW), ((0, 16), (1, 2)), -0.2, 0.2)), 0.25, 2.0)
    output_first = draw_output_first(jax.random.fold_in(keys[12], 71), 0)
    output_second = jnp.clip(jnp.exp(math.log(2.0) - 2.0794415 * jax.random.uniform(keys[11], (R, D), jnp.float32) ** level_of(keys[11], (R, D), ((0, 16), (1, 2)), -0.2, 0.2)), 0.25, 2.0)
    return dict(query_input=query_input, query_cotangent=query_cotangent, branch_output=branch_output, layer_cotangent=layer_cotangent, query_weight=query_weight, output_weight=output_weight, query_basis=query_basis, output_basis=output_basis, query_first=query_first, query_second=query_second, output_first=output_first, output_second=output_second)


beta_first = 0.6
beta_second = 0.8
step_rate = 0.01
small_eps = 1e-06

def project(inputs, basis, cotangent):
    inner = jnp.dot(inputs.astype(jnp.float32), basis.astype(jnp.float32), precision=lax.Precision.HIGHEST, preferred_element_type=jnp.float32)
    return jnp.dot(inner.T, cotangent.astype(jnp.float32), precision=lax.Precision.HIGHEST, preferred_element_type=jnp.float32)

def advance(first, second, projected, basis, weight):
    first_next = beta_first * first + (1.0 - beta_first) * projected
    second_next = beta_second * second + (1.0 - beta_second) * projected * projected
    normed = first_next / jnp.sqrt(second_next)
    scale = lax.rsqrt(jnp.mean(normed * normed) + small_eps)
    rounded = normed.astype(jnp.bfloat16)
    update = scale * jnp.dot(basis.astype(jnp.float32), rounded.astype(jnp.float32), precision=lax.Precision.HIGHEST, preferred_element_type=jnp.float32)
    copy = (weight - step_rate * update).astype(jnp.bfloat16)
    return (update, first_next, second_next, copy)

def reference(query_input, query_cotangent, branch_output, layer_cotangent, query_weight, output_weight, query_basis, output_basis, query_first, query_second, output_first, output_second):
    projected_q = project(query_input, query_basis, query_cotangent)
    projected_o = project(branch_output, output_basis, layer_cotangent)
    update_q, first_q, second_q, copy_q = advance(query_first, query_second, projected_q, query_basis, query_weight)
    update_o, first_o, second_o, copy_o = advance(output_first, output_second, projected_o, output_basis, output_weight)
    return (update_q, update_o, first_q, second_q, first_o, second_o, copy_q, copy_o)
```

```python
import functools

import jax
import jax.numpy as jnp
from jax import lax
from jax.experimental import pallas as pl
from jax.experimental.pallas import tpu as pltpu
from jax.sharding import PartitionSpec as P

MESH = pl.DeviceIdType.MESH
DMA = pltpu.SemaphoreType.DMA

beta_first = 0.6
beta_second = 0.8
step_rate = 0.01
small_eps = 1e-06


def here():
    return lax.axis_index("fs"), lax.axis_index("rep"), lax.axis_index("tp")


def flip(rep, bit):
    if bit == 1:
        return rep + 1 - 2 * lax.rem(rep, 2)
    return lax.rem(rep + 2, 4)


def remote(src, dst, send, recv, device):
    return pltpu.make_async_remote_copy(
        src_ref=src, dst_ref=dst, send_sem=send, recv_sem=recv, device_id=device, device_id_type=MESH
    )


def greet(devices):
    barrier = pltpu.get_barrier_semaphore()
    count = 0
    for device, present in devices:
        if present is True:
            pl.semaphore_signal(barrier, inc=1, device_id=device, device_id_type=MESH)
            count = count + 1
        else:
            count = count + present.astype(jnp.int32)

            @pl.when(present)
            def _():
                pl.semaphore_signal(barrier, inc=1, device_id=device, device_id_type=MESH)

    pl.semaphore_wait(barrier, count)


class Line:
    def __init__(self, n, view, send, recv):
        self.n, self.view, self.send_sem, self.recv_sem = n, view, send, recv
        self.fs, self.rep, self.tp = here()

    def outgoing(self, step, way):
        fs, n = self.fs, self.n
        if way == 0:
            block, peer = fs - step + 1, fs + 1
            present = jnp.logical_and(block >= 0, peer < n)
        else:
            block, peer = fs + step - 1, fs - 1
            present = jnp.logical_and(block < n, peer >= 0)
        block = lax.rem(block + n, n)
        peer = lax.rem(peer + n, n)
        view = self.view(block)
        sems = (self.send_sem.at[way, step - 1], self.recv_sem.at[way, step - 1])
        return remote(view, view, *sems, (peer, self.rep, self.tp)), present

    def incoming(self, step, way):
        fs, n = self.fs, self.n
        block = fs - step if way == 0 else fs + step
        present = block >= 0 if way == 0 else block < n
        block = lax.rem(block + n, n)
        view = self.view(block)
        sems = (self.send_sem.at[way, step - 1], self.recv_sem.at[way, step - 1])
        return remote(view, view, *sems, (fs, self.rep, self.tp)), present, block

    def start(self, step):
        for way in (0, 1):
            copy, present = self.outgoing(step, way)

            @pl.when(present)
            def _():
                copy.start()

    def arrive(self, step):
        for way in (0, 1):
            copy, present, _ = self.incoming(step, way)

            @pl.when(present)
            def _():
                copy.wait_recv()

    def sent(self):
        for step in range(1, self.n):
            for way in (0, 1):
                copy, present = self.outgoing(step, way)

                @pl.when(present)
                def _():
                    copy.wait_send()


def gather(n, views, line_sems, one_sems, two_sems, third_sems=None, between=None):
    fs, rep, tp = here()
    lines = [
        Line(n, lambda b, v=v: v(rep * n + b, None), line_sems[0].at[a], line_sems[1].at[a])
        for a, v in enumerate(views)
    ]
    bits = ((1, 2), (2, 1))

    def slots():
        yield 0, 0, 0
        for step in range(1, n):
            yield step, 0, 2 * step - 1
            yield step, 1, 2 * step

    def block_of(step, way):
        if step == 0:
            return fs, True
        block = fs - step if way == 0 else fs + step
        present = block >= 0 if way == 0 else block < n
        return lax.rem(block + n, n), present

    def when(present, body):
        if present is True:
            body()
        else:
            pl.when(present)(body)

    def one(a, block, slot, half):
        peer = flip(rep, bits[half][0])
        view = views[a](rep * n + block, half)
        return remote(view, view, one_sems[0].at[a, half, slot], one_sems[1].at[a, half, slot], (fs, peer, tp))

    def one_in(a, block, slot, half):
        peer = flip(rep, bits[half][0])
        view = views[a](peer * n + block, half)
        return remote(view, view, one_sems[0].at[a, half, slot], one_sems[1].at[a, half, slot], (fs, peer, tp))

    def two(a, block, slot, half, which):
        peer = flip(rep, bits[half][1])
        held = rep if which == 0 else flip(rep, bits[half][0])
        view = views[a](held * n + block, half)
        sems = [s.at[a, half, which, slot] for s in two_sems]
        return remote(view, view, *sems, (fs, peer, tp))

    def two_in(a, block, slot, half, which):
        peer = flip(rep, bits[half][1])
        held = peer if which == 0 else flip(peer, bits[half][0])
        view = views[a](held * n + block, half)
        sems = [s.at[a, half, which, slot] for s in two_sems]
        return remote(view, view, *sems, (fs, peer, tp))

    def third(a, block, group):
        view = views[a](group * n + block, None)
        sems = [s.at[a, group, block] for s in third_sems]
        return remote(view, view, *sems, (fs, rep, 1 - tp))

    def third_in(a, block, group):
        view = views[a](group * n + block, None, 1 - tp)
        sems = [s.at[a, group, block] for s in third_sems]
        return remote(view, view, *sems, (fs, rep, 1 - tp))

    arrays = range(len(views))

    def launch(step, way, slot):
        block, present = block_of(step, way)

        def body():
            for a in arrays:
                for half in (0, 1):
                    one(a, block, slot, half).start()
                for half in (0, 1):
                    two(a, block, slot, half, 0).start()

        when(present, body)

    def relay(step, way, slot):
        block, present = block_of(step, way)

        def body():
            for a in arrays:
                for half in (0, 1):
                    one_in(a, block, slot, half).wait_recv()
                    two(a, block, slot, half, 1).start()

        when(present, body)

    def finish(step, way, slot):
        block, present = block_of(step, way)

        def body():
            for a in arrays:
                for half in (0, 1):
                    for which in (0, 1):
                        two_in(a, block, slot, half, which).wait_recv()
                if third_sems is not None:
                    for group in range(4):
                        third(a, block, group).start()

        when(present, body)

    def drain(step, way, slot):
        block, present = block_of(step, way)

        def body():
            for a in arrays:
                for half in (0, 1):
                    one(a, block, slot, half).wait_send()
                    for which in (0, 1):
                        two(a, block, slot, half, which).wait_send()
                if third_sems is not None:
                    for group in range(4):
                        third(a, block, group).wait_send()
                        third_in(a, block, group).wait_recv()

        when(present, body)

    order = list(slots())
    for step in range(n):
        if step:
            for line in lines:
                line.arrive(step)
        if step < n - 1:
            for line in lines:
                line.start(step + 1)
        if step == 0 and between is not None:
            between()
        for s, way, slot in order:
            if s == step:
                launch(s, way, slot)
        for s, way, slot in order:
            if s == step - 1:
                relay(s, way, slot)
    for s, way, slot in order:
        if s == n - 1:
            relay(s, way, slot)
    for s, way, slot in order:
        finish(s, way, slot)
    for s, way, slot in order:
        drain(s, way, slot)
    for line in lines:
        line.sent()


def pairs(*shapes):
    return [DMA(shape) for shape in shapes for _ in (0, 1)]


def first_kernel(
    n, bq_ref, bo_ref, w_ref, gq_ref, go_ref, gw_ref,
    local, ls, lr, os, orr, ts, tr, hs, hr, ws, wr,
):
    fs, rep, tp = here()
    mine = rep * n + fs
    copies = [
        pltpu.make_async_copy(bq_ref, gq_ref.at[mine], local.at[0]),
        pltpu.make_async_copy(bo_ref, go_ref.at[mine], local.at[1]),
        pltpu.make_async_copy(w_ref, gw_ref.at[fs], local.at[2]),
    ]
    for copy in copies:
        copy.start()
    peers = [((lax.rem(fs + 1, n), rep, tp), fs + 1 < n), ((lax.rem(fs + n - 1, n), rep, tp), fs >= 1)]
    peers += [((fs, flip(rep, bit), tp), True) for bit in (1, 2)]
    peers += [((fs, rep, 1 - tp), True)]
    for copy in copies:
        copy.wait()
    greet(peers)

    def view_of(ref):
        rows, cols = ref.shape[1] // 2, ref.shape[2] // 2

        def view(block, half, core=None):
            core = tp if core is None else core
            span = pl.ds(pl.multiple_of(core * cols, cols), cols)
            if half is None:
                return ref.at[block, :, span]
            return ref.at[block, pl.ds(half * rows, rows), span]

        return view

    weights = Line(n, lambda b: gw_ref.at[b], ws, wr)
    gather(
        n, [view_of(gq_ref), view_of(go_ref)], (ls, lr), (os, orr), (ts, tr), (hs, hr),
        between=lambda: weights.start(1),
    )
    for step in range(1, n):
        weights.arrive(step)
        if step < n - 1:
            weights.start(step + 1)
    weights.sent()


def gather_bases(n, basis_q, basis_o, weight):
    slots = 2 * n - 1
    whole = lambda a: jax.ShapeDtypeStruct((4 * n, *a.shape), a.dtype)
    vmem = pl.BlockSpec(memory_space=pltpu.VMEM)
    return pl.pallas_call(
        functools.partial(first_kernel, n),
        out_shape=(whole(basis_q), whole(basis_o), jax.ShapeDtypeStruct((n, *weight.shape), weight.dtype)),
        in_specs=[vmem] * 3,
        out_specs=(vmem,) * 3,
        scratch_shapes=[DMA((3,))]
        + pairs((2, 2, n - 1), (2, 2, slots), (2, 2, 2, slots), (2, 4, n), (2, n - 1)),
        compiler_params=pltpu.CompilerParams(
            collective_id=0, has_side_effects=True, vmem_limit_bytes=40 * 2**20
        ),
        name="gather_bases",
    )(basis_q, basis_o, weight)


def second_kernel(
    n, pq_ref, po_ref, fq_ref, sq_ref, fo_ref, so_ref, w_ref,
    nfq_ref, nsq_ref, nfo_ref, nso_ref, gq_ref, go_ref, gw_ref, tot_ref,
    rq, ro, aq, ao, zq, zo, gs, local,
    rs, rr, zs, zr, ls, lr, os, orr, ts, tr, ws, wr, cs, cr,
):
    fs, rep, tp = here()
    mine = rep * n + fs
    own = pltpu.make_async_copy(w_ref, gw_ref.at[fs], local.at[0])
    own.start()
    peers = [((lax.rem(fs + k, n), rep, tp), True) for k in range(1, n)]
    peers += [((fs, lax.rem(rep + k, 4), tp), True) for k in range(1, 4)]
    peers += [((fs, rep, 1 - tp), True)]
    own.wait()
    greet(peers)
    weights = Line(n, lambda b: gw_ref.at[b], ws, wr)

    parts, heard, summed, late = (pq_ref, po_ref), (rq, ro), (aq, ao), (zq, zo)

    def swap(a, j, k):
        f, to = lax.rem(fs + j, n), lax.rem(rep + k, 4)
        sems = (rs.at[a, j - 1, k - 1], rr.at[a, j - 1, k - 1])
        return remote(parts[a].at[to * n + f], heard[a].at[j - 1, k - 1], *sems, (fs, to, tp))

    def cross(a, j):
        f = lax.rem(fs + j, n)
        return remote(
            summed[a].at[j - 1], late[a].at[j - 1], zs.at[a, j - 1], zr.at[a, j - 1], (f, rep, tp)
        )

    for j in range(1, n + 1):
        for a in (1, 0):
            for k in (2, 1, 3):
                swap(a, j, k).start()
    weights.start(1)
    final = [None, None]
    for j in range(1, n + 1):
        f = lax.rem(fs + j, n)
        for a in (1, 0):
            for k in (2, 1, 3):
                swap(a, j, k).wait_recv()
            total = parts[a][rep * n + f].astype(jnp.float32)
            for k in (1, 2, 3):
                total = total + heard[a][j - 1, k - 1].astype(jnp.float32)
            if j < n:
                summed[a][j - 1] = total.astype(jnp.bfloat16)
                cross(a, j).start()
            else:
                final[a] = total
    for a in (0, 1):
        for j in range(1, n):
            cross(a, j).wait_recv()
        for j in range(1, n):
            final[a] = final[a] + late[a][j - 1].astype(jnp.float32)
    refs = ((fq_ref, sq_ref, nfq_ref, nsq_ref, gq_ref), (fo_ref, so_ref, nfo_ref, nso_ref, go_ref))
    for a in (0, 1):
        first, second, first_out, second_out, g = refs[a]
        first_next = beta_first * first[...] + (1.0 - beta_first) * final[a]
        second_next = beta_second * second[...] + (1.0 - beta_second) * final[a] * final[a]
        normed = first_next / jnp.sqrt(second_next)
        first_out[...] = first_next
        second_out[...] = second_next
        g[mine] = normed.astype(jnp.bfloat16)
        square = normed * normed
        rows, cols = square.shape
        square = sum(square[:, c : c + 128] for c in range(0, cols, 128))
        square = sum(square[r : r + 8] for r in range(0, rows, 8))
        gs[mine, :, a * 128 : (a + 1) * 128] = square

    def view_of(ref):
        cols = ref.shape[2] // 2

        def view(block, half):
            if half is None:
                return ref.at[block]
            return ref.at[block, :, pl.ds(half * cols, cols)]

        return view

    gather(n, [view_of(go_ref), view_of(gq_ref), view_of(gs)], (ls, lr), (os, orr), (ts, tr))
    for step in range(1, n):
        weights.arrive(step)
        if step < n - 1:
            weights.start(step + 1)
    tot_ref[0] = sum(gs[b] for b in range(4 * n))
    pair = remote(tot_ref.at[0], tot_ref.at[1], cs.at[0], cr.at[0], (fs, rep, 1 - tp))
    pair.start()
    pair.wait()
    weights.sent()
    for j in range(1, n + 1):
        for a in (0, 1):
            for k in (1, 2, 3):
                swap(a, j, k).wait_send()
            if j < n:
                cross(a, j).wait_send()


def advance(n, part_q, part_o, first_q, second_q, first_o, second_o, weight):
    slots = 2 * n - 1
    rows, cq = first_q.shape
    co = first_o.shape[1]
    f32, b16 = jnp.float32, jnp.bfloat16
    shape = jax.ShapeDtypeStruct
    vmem = pl.BlockSpec(memory_space=pltpu.VMEM)
    return pl.pallas_call(
        functools.partial(second_kernel, n),
        out_shape=(
            shape((rows, cq), f32), shape((rows, cq), f32), shape((rows, co), f32), shape((rows, co), f32),
            shape((4 * n, rows, cq), b16), shape((4 * n, rows, co), b16),
            shape((n, *weight.shape), b16), shape((2, 8, 256), f32),
        ),
        in_specs=[vmem] * 7,
        out_specs=(vmem,) * 8,
        scratch_shapes=[
            pltpu.VMEM((n, 3, rows, cq), b16), pltpu.VMEM((n, 3, rows, co), b16),
            pltpu.VMEM((n - 1, rows, cq), b16), pltpu.VMEM((n - 1, rows, co), b16),
            pltpu.VMEM((n - 1, rows, cq), b16), pltpu.VMEM((n - 1, rows, co), b16),
            pltpu.VMEM((4 * n, 8, 256), f32), DMA((1,)),
        ]
        + pairs((2, n, 3), (2, n - 1), (3, 2, n - 1), (3, 2, slots), (3, 2, 2, slots), (2, n - 1), (1,)),
        compiler_params=pltpu.CompilerParams(
            collective_id=1, has_side_effects=True, vmem_limit_bytes=48 * 2**20
        ),
        name="advance",
    )(part_q, part_o, first_q, second_q, first_o, second_o, weight)


def body(
    n,
    query_input,
    query_cotangent,
    branch_output,
    layer_cotangent,
    query_weight,
    output_weight,
    query_basis,
    output_basis,
    query_first,
    query_second,
    output_first,
    output_second,
):
    f32, b16 = jnp.float32, jnp.bfloat16
    rank = query_basis.shape[1]
    gq, go, wq = gather_bases(n, query_basis, output_basis, query_weight.astype(b16))
    whole_q, whole_o = gq.reshape(-1, rank), go.reshape(-1, rank)

    def project(inputs, basis, cotangent):
        inner = jnp.dot(inputs, basis, preferred_element_type=f32).astype(b16)
        part = lax.dot_general(inner, cotangent, (((0,), (0,)), ((), ())), preferred_element_type=f32)
        return part.astype(b16).reshape(4 * n, -1, cotangent.shape[1])

    part_q = project(query_input, whole_q, query_cotangent)
    part_o = project(branch_output, whole_o, layer_cotangent)
    first_q, second_q, first_o, second_o, nq, no, wo, totals = advance(
        n, part_q, part_o, query_first, query_second, output_first, output_second, output_weight.astype(b16)
    )
    sums = jnp.sum(totals.reshape(16, 2, 128), axis=(0, 2))
    rep = lax.axis_index("rep")

    def update(basis, whole, normed, total, weights):
        normed = normed.reshape(rank, -1)
        columns = normed.shape[1]
        scale = lax.rsqrt(total / (rank * 2 * columns) + small_eps)
        mine = scale * jnp.dot(basis, normed, preferred_element_type=f32)
        weights = weights.reshape(-1, columns)
        count = weights.shape[0]
        rows = lax.dynamic_slice_in_dim(whole, rep * count, count)
        group = scale * jnp.dot(rows, normed, preferred_element_type=f32)
        return mine, (weights.astype(f32) - step_rate * group).astype(b16)

    update_q, copy_q = update(query_basis, whole_q, nq, sums[0], wq)
    update_o, copy_o = update(output_basis, whole_o, no, sums[1], wo)
    return (update_q, update_o, first_q, second_q, first_o, second_o, copy_q, copy_o)


def solution(mesh):
    in_specs = (
        P(("fs", "rep"), None),
        P(("fs", "rep"), "tp"),
        P(("fs", "rep"), None),
        P(("fs", "rep"), "tp"),
        P(("rep", "fs"), "tp"),
        P(("rep", "fs"), "tp"),
        P(("rep", "fs"), None),
        P(("rep", "fs"), None),
        P(("rep", "fs"), "tp"),
        P(("rep", "fs"), "tp"),
        P(("rep", "fs"), "tp"),
        P(("rep", "fs"), "tp"),
    )
    out_specs = (
        P(("rep", "fs"), "tp"),
        P(("rep", "fs"), "tp"),
        P(("rep", "fs"), "tp"),
        P(("rep", "fs"), "tp"),
        P(("rep", "fs"), "tp"),
        P(("rep", "fs"), "tp"),
        P("rep", "tp"),
        P("rep", "tp"),
    )
    n = mesh.shape["fs"]
    assert mesh.shape["rep"] == 4 and mesh.shape["tp"] == 2
    return jax.shard_map(functools.partial(body, n), mesh=mesh, in_specs=in_specs, out_specs=out_specs, check_vma=False)
```

```python
import functools

import jax
import jax.numpy as jnp
from jax import lax
from jax.experimental import pallas as pl
from jax.experimental.pallas import tpu as pltpu
from jax.sharding import PartitionSpec as P

MESH = pl.DeviceIdType.MESH
DMA = pltpu.SemaphoreType.DMA

beta_first = 0.6
beta_second = 0.8
step_rate = 0.01
small_eps = 1e-06


def here():
    return lax.axis_index("fs"), lax.axis_index("rep"), lax.axis_index("tp")


def flip(rep, bit):
    if bit == 1:
        return rep + 1 - 2 * lax.rem(rep, 2)
    return lax.rem(rep + 2, 4)


def remote(src, dst, send, recv, device):
    return pltpu.make_async_remote_copy(
        src_ref=src, dst_ref=dst, send_sem=send, recv_sem=recv, device_id=device, device_id_type=MESH
    )


def greet(devices):
    barrier = pltpu.get_barrier_semaphore()
    count = 0
    for device, present in devices:
        if present is True:
            pl.semaphore_signal(barrier, inc=1, device_id=device, device_id_type=MESH)
            count = count + 1
        else:
            count = count + present.astype(jnp.int32)

            @pl.when(present)
            def _():
                pl.semaphore_signal(barrier, inc=1, device_id=device, device_id_type=MESH)

    pl.semaphore_wait(barrier, count)


class Line:
    def __init__(self, n, view, send, recv):
        self.n, self.view, self.send_sem, self.recv_sem = n, view, send, recv
        self.fs, self.rep, self.tp = here()
        self.done = 0

    def tick(self):
        if 0 < self.done < self.n:
            self.arrive(self.done)
        if self.done + 1 < self.n:
            self.start(self.done + 1)
        self.done += 1

    def outgoing(self, step, way):
        fs, n = self.fs, self.n
        if way == 0:
            block, peer = fs - step + 1, fs + 1
            present = jnp.logical_and(block >= 0, peer < n)
        else:
            block, peer = fs + step - 1, fs - 1
            present = jnp.logical_and(block < n, peer >= 0)
        block = lax.rem(block + n, n)
        peer = lax.rem(peer + n, n)
        view = self.view(block)
        sems = (self.send_sem.at[way, step - 1], self.recv_sem.at[way, step - 1])
        return remote(view, view, *sems, (peer, self.rep, self.tp)), present

    def incoming(self, step, way):
        fs, n = self.fs, self.n
        block = fs - step if way == 0 else fs + step
        present = block >= 0 if way == 0 else block < n
        block = lax.rem(block + n, n)
        view = self.view(block)
        sems = (self.send_sem.at[way, step - 1], self.recv_sem.at[way, step - 1])
        return remote(view, view, *sems, (fs, self.rep, self.tp)), present, block

    def start(self, step):
        for way in (0, 1):
            copy, present = self.outgoing(step, way)

            @pl.when(present)
            def _():
                copy.start()

    def arrive(self, step):
        for way in (0, 1):
            copy, present, _ = self.incoming(step, way)

            @pl.when(present)
            def _():
                copy.wait_recv()

    def sent(self):
        for step in range(1, self.n):
            for way in (0, 1):
                copy, present = self.outgoing(step, way)

                @pl.when(present)
                def _():
                    copy.wait_send()


def gather(n, views, line_sems, one_sems, two_sems, third_sems=None, ticks=()):
    fs, rep, tp = here()
    lines = [
        Line(n, lambda b, v=v: v(rep * n + b, None), line_sems[0].at[a], line_sems[1].at[a])
        for a, v in enumerate(views)
    ]
    bits = ((1, 2), (2, 1))

    def slots():
        yield 0, 0, 0
        for step in range(1, n):
            yield step, 0, 2 * step - 1
            yield step, 1, 2 * step

    def block_of(step, way):
        if step == 0:
            return fs, True
        block = fs - step if way == 0 else fs + step
        present = block >= 0 if way == 0 else block < n
        return lax.rem(block + n, n), present

    def when(present, body):
        if present is True:
            body()
        else:
            pl.when(present)(body)

    def one(a, block, slot, half):
        peer = flip(rep, bits[half][0])
        view = views[a](rep * n + block, half)
        return remote(view, view, one_sems[0].at[a, half, slot], one_sems[1].at[a, half, slot], (fs, peer, tp))

    def one_in(a, block, slot, half):
        peer = flip(rep, bits[half][0])
        view = views[a](peer * n + block, half)
        return remote(view, view, one_sems[0].at[a, half, slot], one_sems[1].at[a, half, slot], (fs, peer, tp))

    def two(a, block, slot, half, which):
        peer = flip(rep, bits[half][1])
        held = rep if which == 0 else flip(rep, bits[half][0])
        view = views[a](held * n + block, half)
        sems = [s.at[a, half, which, slot] for s in two_sems]
        return remote(view, view, *sems, (fs, peer, tp))

    def two_in(a, block, slot, half, which):
        peer = flip(rep, bits[half][1])
        held = peer if which == 0 else flip(peer, bits[half][0])
        view = views[a](held * n + block, half)
        sems = [s.at[a, half, which, slot] for s in two_sems]
        return remote(view, view, *sems, (fs, peer, tp))

    def third(a, block, group):
        view = views[a](group * n + block, None)
        sems = [s.at[a, group, block] for s in third_sems]
        return remote(view, view, *sems, (fs, rep, 1 - tp))

    def third_in(a, block, group):
        view = views[a](group * n + block, None, 1 - tp)
        sems = [s.at[a, group, block] for s in third_sems]
        return remote(view, view, *sems, (fs, rep, 1 - tp))

    arrays = range(len(views))

    def launch(step, way, slot):
        block, present = block_of(step, way)

        def body():
            for a in arrays:
                for half in (0, 1):
                    one(a, block, slot, half).start()
                for half in (0, 1):
                    two(a, block, slot, half, 0).start()

        when(present, body)

    def relay(step, way, slot):
        block, present = block_of(step, way)

        def body():
            for a in arrays:
                for half in (0, 1):
                    one_in(a, block, slot, half).wait_recv()
                    two(a, block, slot, half, 1).start()

        when(present, body)

    def finish(step, way, slot):
        block, present = block_of(step, way)

        def body():
            for a in arrays:
                for half in (0, 1):
                    for which in (0, 1):
                        two_in(a, block, slot, half, which).wait_recv()
                if third_sems is not None:
                    for group in range(4):
                        third(a, block, group).start()

        when(present, body)

    def drain(step, way, slot):
        block, present = block_of(step, way)

        def body():
            for a in arrays:
                for half in (0, 1):
                    one(a, block, slot, half).wait_send()
                    for which in (0, 1):
                        two(a, block, slot, half, which).wait_send()
                if third_sems is not None:
                    for group in range(4):
                        third(a, block, group).wait_send()
                        third_in(a, block, group).wait_recv()

        when(present, body)

    order = list(slots())
    for step in range(n):
        if step:
            for line in lines:
                line.arrive(step)
        if step < n - 1:
            for line in lines:
                line.start(step + 1)
        if step == n - 2:
            for side in ticks:
                side.tick()
        for s, way, slot in order:
            if s == step:
                launch(s, way, slot)
        for s, way, slot in order:
            if s == step - 1:
                relay(s, way, slot)
            if s == step - 2:
                finish(s, way, slot)
    for side in ticks:
        side.tick()
    for s, way, slot in order:
        if s == n - 1:
            relay(s, way, slot)
        if s == n - 2:
            finish(s, way, slot)
    for side in ticks:
        side.tick()
    for s, way, slot in order:
        if s == n - 1:
            finish(s, way, slot)
    for side in ticks:
        while side.done < n:
            side.tick()
    for s, way, slot in order:
        drain(s, way, slot)
    for line in lines:
        line.sent()


def pairs(*shapes):
    return [DMA(shape) for shape in shapes for _ in (0, 1)]


def first_kernel(
    n, bq_ref, bo_ref, w_ref, v_ref, gq_ref, go_ref, gw_ref, gv_ref,
    local, ls, lr, os, orr, ts, tr, hs, hr, ws, wr,
):
    fs, rep, tp = here()
    mine = rep * n + fs
    copies = [
        pltpu.make_async_copy(bq_ref, gq_ref.at[mine], local.at[0]),
        pltpu.make_async_copy(bo_ref, go_ref.at[mine], local.at[1]),
        pltpu.make_async_copy(w_ref, gw_ref.at[fs], local.at[2]),
        pltpu.make_async_copy(v_ref, gv_ref.at[fs], local.at[3]),
    ]
    for copy in copies:
        copy.start()
    peers = [((lax.rem(fs + 1, n), rep, tp), fs + 1 < n), ((lax.rem(fs + n - 1, n), rep, tp), fs >= 1)]
    peers += [((fs, flip(rep, bit), tp), True) for bit in (1, 2)]
    peers += [((fs, rep, 1 - tp), True)]
    for copy in copies:
        copy.wait()
    greet(peers)

    def view_of(ref):
        rows, cols = ref.shape[1] // 2, ref.shape[2] // 2

        def view(block, half, core=None):
            core = tp if core is None else core
            span = pl.ds(pl.multiple_of(core * cols, cols), cols)
            if half is None:
                return ref.at[block, :, span]
            return ref.at[block, pl.ds(half * rows, rows), span]

        return view

    weights = [
        Line(n, lambda b, g=g: g.at[b], ws.at[i], wr.at[i]) for i, g in enumerate((gw_ref, gv_ref))
    ]
    gather(
        n, [view_of(gq_ref), view_of(go_ref)], (ls, lr), (os, orr), (ts, tr), (hs, hr), ticks=weights
    )
    for side in weights:
        side.sent()


def gather_bases(n, basis_q, basis_o, *weights):
    slots = 2 * n - 1
    whole = lambda a: jax.ShapeDtypeStruct((4 * n, *a.shape), a.dtype)
    vmem = pl.BlockSpec(memory_space=pltpu.VMEM)
    return pl.pallas_call(
        functools.partial(first_kernel, n),
        out_shape=(whole(basis_q), whole(basis_o))
        + tuple(jax.ShapeDtypeStruct((n, *w.shape), w.dtype) for w in weights),
        in_specs=[vmem] * 4,
        out_specs=(vmem,) * 4,
        scratch_shapes=[DMA((4,))]
        + pairs((2, 2, n - 1), (2, 2, slots), (2, 2, 2, slots), (2, 4, n), (2, 2, n - 1)),
        compiler_params=pltpu.CompilerParams(
            collective_id=0, has_side_effects=True, vmem_limit_bytes=40 * 2**20
        ),
        name="gather_bases",
    )(basis_q, basis_o, *weights)


def second_kernel(
    n, pq_ref, po_ref, fq_ref, sq_ref, fo_ref, so_ref, w_ref,
    nfq_ref, nsq_ref, nfo_ref, nso_ref, gq_ref, go_ref, gw_ref, tot_ref,
    rq, ro, aq, ao, zq, zo, gs, local,
    rs, rr, zs, zr, ls, lr, os, orr, ts, tr, ws, wr, cs, cr,
):
    fs, rep, tp = here()
    mine = rep * n + fs
    own = pltpu.make_async_copy(w_ref, gw_ref.at[fs], local.at[0])
    own.start()
    peers = [((lax.rem(fs + k, n), rep, tp), True) for k in range(1, n)]
    peers += [((fs, lax.rem(rep + k, 4), tp), True) for k in range(1, 4)]
    peers += [((fs, rep, 1 - tp), True)]
    own.wait()
    greet(peers)
    weights = Line(n, lambda b: gw_ref.at[b], ws, wr)

    parts, heard, summed, late = (pq_ref, po_ref), (rq, ro), (aq, ao), (zq, zo)

    def swap(a, j, k):
        f, to = lax.rem(fs + j, n), lax.rem(rep + k, 4)
        sems = (rs.at[a, j - 1, k - 1], rr.at[a, j - 1, k - 1])
        return remote(parts[a].at[to * n + f], heard[a].at[j - 1, k - 1], *sems, (fs, to, tp))

    def cross(a, j):
        f = lax.rem(fs + j, n)
        return remote(
            summed[a].at[j - 1], late[a].at[j - 1], zs.at[a, j - 1], zr.at[a, j - 1], (f, rep, tp)
        )

    for j in range(1, n + 1):
        for a in (1, 0):
            for k in (2, 1, 3):
                swap(a, j, k).start()
    weights.tick()
    final = [None, None]
    for j in range(1, n + 1):
        f = lax.rem(fs + j, n)
        for a in (1, 0):
            for k in (2, 1, 3):
                swap(a, j, k).wait_recv()
            total = parts[a][rep * n + f].astype(jnp.float32)
            for k in (1, 2, 3):
                total = total + heard[a][j - 1, k - 1].astype(jnp.float32)
            if j < n:
                summed[a][j - 1] = total.astype(jnp.bfloat16)
                cross(a, j).start()
            else:
                final[a] = total
    for a in (0, 1):
        for j in range(1, n):
            cross(a, j).wait_recv()
        for j in range(1, n):
            final[a] = final[a] + late[a][j - 1].astype(jnp.float32)
    refs = ((fq_ref, sq_ref, nfq_ref, nsq_ref, gq_ref), (fo_ref, so_ref, nfo_ref, nso_ref, go_ref))
    for a in (0, 1):
        first, second, first_out, second_out, g = refs[a]
        first_next = beta_first * first[...] + (1.0 - beta_first) * final[a]
        second_next = beta_second * second[...] + (1.0 - beta_second) * final[a] * final[a]
        normed = first_next / jnp.sqrt(second_next)
        first_out[...] = first_next
        second_out[...] = second_next
        g[mine] = normed.astype(jnp.bfloat16)
        square = normed * normed
        rows, cols = square.shape
        square = sum(square[:, c : c + 128] for c in range(0, cols, 128))
        square = sum(square[r : r + 8] for r in range(0, rows, 8))
        gs[mine, :, a * 128 : (a + 1) * 128] = square

    def view_of(ref):
        cols = ref.shape[2] // 2

        def view(block, half):
            if half is None:
                return ref.at[block]
            return ref.at[block, :, pl.ds(half * cols, cols)]

        return view

    gather(n, [view_of(go_ref), view_of(gq_ref), view_of(gs)], (ls, lr), (os, orr), (ts, tr), ticks=[weights])
    tot_ref[0] = sum(gs[b] for b in range(4 * n))
    pair = remote(tot_ref.at[0], tot_ref.at[1], cs.at[0], cr.at[0], (fs, rep, 1 - tp))
    pair.start()
    pair.wait()
    weights.sent()
    for j in range(1, n + 1):
        for a in (0, 1):
            for k in (1, 2, 3):
                swap(a, j, k).wait_send()
            if j < n:
                cross(a, j).wait_send()


def advance(n, part_q, part_o, first_q, second_q, first_o, second_o, weight):
    slots = 2 * n - 1
    rows, cq = first_q.shape
    co = first_o.shape[1]
    f32, b16 = jnp.float32, jnp.bfloat16
    shape = jax.ShapeDtypeStruct
    vmem = pl.BlockSpec(memory_space=pltpu.VMEM)
    return pl.pallas_call(
        functools.partial(second_kernel, n),
        out_shape=(
            shape((rows, cq), f32), shape((rows, cq), f32), shape((rows, co), f32), shape((rows, co), f32),
            shape((4 * n, rows, cq), b16), shape((4 * n, rows, co), b16),
            shape((n, *weight.shape), b16), shape((2, 8, 256), f32),
        ),
        in_specs=[vmem] * 7,
        out_specs=(vmem,) * 8,
        scratch_shapes=[
            pltpu.VMEM((n, 3, rows, cq), b16), pltpu.VMEM((n, 3, rows, co), b16),
            pltpu.VMEM((n - 1, rows, cq), b16), pltpu.VMEM((n - 1, rows, co), b16),
            pltpu.VMEM((n - 1, rows, cq), b16), pltpu.VMEM((n - 1, rows, co), b16),
            pltpu.VMEM((4 * n, 8, 256), f32), DMA((1,)),
        ]
        + pairs((2, n, 3), (2, n - 1), (3, 2, n - 1), (3, 2, slots), (3, 2, 2, slots), (2, n - 1), (1,)),
        compiler_params=pltpu.CompilerParams(
            collective_id=1, has_side_effects=True, vmem_limit_bytes=48 * 2**20
        ),
        name="advance",
    )(part_q, part_o, first_q, second_q, first_o, second_o, weight)


def body(
    n,
    query_input,
    query_cotangent,
    branch_output,
    layer_cotangent,
    query_weight,
    output_weight,
    query_basis,
    output_basis,
    query_first,
    query_second,
    output_first,
    output_second,
):
    f32, b16 = jnp.float32, jnp.bfloat16
    rank = query_basis.shape[1]
    half = output_weight.shape[0] // 2
    near, far = output_weight[:half].astype(b16), output_weight[half:].astype(b16)
    gq, go, wq, wo_near = gather_bases(n, query_basis, output_basis, query_weight.astype(b16), near)
    whole_q, whole_o = gq.reshape(-1, rank), go.reshape(-1, rank)

    def project(inputs, basis, cotangent):
        inner = jnp.dot(inputs, basis, preferred_element_type=f32).astype(b16)
        part = lax.dot_general(inner, cotangent, (((0,), (0,)), ((), ())), preferred_element_type=f32)
        return part.astype(b16).reshape(4 * n, -1, cotangent.shape[1])

    part_q = project(query_input, whole_q, query_cotangent)
    part_o = project(branch_output, whole_o, layer_cotangent)
    first_q, second_q, first_o, second_o, nq, no, wo_far, totals = advance(
        n, part_q, part_o, query_first, query_second, output_first, output_second, far
    )
    sums = jnp.sum(totals.reshape(16, 2, 128), axis=(0, 2))
    rep = lax.axis_index("rep")

    def update(basis, whole, normed, total, weights):
        normed = normed.reshape(rank, -1)
        columns = normed.shape[1]
        scale = lax.rsqrt(total / (rank * 2 * columns) + small_eps)
        mine = scale * jnp.dot(basis, normed, preferred_element_type=f32)
        weights = weights.reshape(-1, columns)
        count = weights.shape[0]
        rows = lax.dynamic_slice_in_dim(whole, rep * count, count)
        group = scale * jnp.dot(rows, normed, preferred_element_type=f32)
        return mine, (weights.astype(f32) - step_rate * group).astype(b16)

    update_q, copy_q = update(query_basis, whole_q, nq, sums[0], wq)
    update_o, copy_o = update(output_basis, whole_o, no, sums[1], jnp.concatenate([wo_near, wo_far], axis=1))
    return (update_q, update_o, first_q, second_q, first_o, second_o, copy_q, copy_o)


def solution(mesh):
    in_specs = (
        P(("fs", "rep"), None),
        P(("fs", "rep"), "tp"),
        P(("fs", "rep"), None),
        P(("fs", "rep"), "tp"),
        P(("rep", "fs"), "tp"),
        P(("rep", "fs"), "tp"),
        P(("rep", "fs"), None),
        P(("rep", "fs"), None),
        P(("rep", "fs"), "tp"),
        P(("rep", "fs"), "tp"),
        P(("rep", "fs"), "tp"),
        P(("rep", "fs"), "tp"),
    )
    out_specs = (
        P(("rep", "fs"), "tp"),
        P(("rep", "fs"), "tp"),
        P(("rep", "fs"), "tp"),
        P(("rep", "fs"), "tp"),
        P(("rep", "fs"), "tp"),
        P(("rep", "fs"), "tp"),
        P("rep", "tp"),
        P("rep", "tp"),
    )
    n = mesh.shape["fs"]
    assert mesh.shape["rep"] == 4 and mesh.shape["tp"] == 2
    return jax.shard_map(functools.partial(body, n), mesh=mesh, in_specs=in_specs, out_specs=out_specs, check_vma=False)
```
